128 devices in a mesh: fs: 16 (over z, x), tp: 8 (over y, core).
Axes of the slice: x: 4, y: 4, z: 4, core: 2. Of those that a mesh axis runs over, the one named last changes fastest.
Arguments:
- seq_rows: bfloat16 [12288, 2048], P('fs', 'tp'), may hold values from -6 to 6
- mixer_gain: bfloat16 [2048], P('tp'), may hold values from 0.099609375 to 1.8984375
- query_weight: bfloat16 [2048, 2048], P('fs', 'tp'), may hold values from -0.125 to 0.125
- key_weight: bfloat16 [2048, 2048], P('fs', 'tp'), may hold values from -0.125 to 0.125
- value_weight: bfloat16 [2048, 4096], P('fs', 'tp'), may hold values from -0.125 to 0.125
- decay_logs: float32 [8], P('tp'), may hold values from -0.0333333333 to -0.000390625
- mixer_out_weight: bfloat16 [4096, 2048], P('tp', 'fs'), may hold values from -0.125 to 0.125
- channel_gain: bfloat16 [2048], P('tp'), may hold values from 0.099609375 to 1.8984375
- value_up_weight: bfloat16 [2048, 5632], P('fs', 'tp'), may hold values from -0.125 to 0.125
- gate_up_weight: bfloat16 [2048, 5632], P('fs', 'tp'), may hold values from -0.125 to 0.125
- conv_taps: bfloat16 [3, 5632], P(None, 'tp'), may hold values from -3 to 3
- conv_bias: bfloat16 [5632], P('tp'), may hold values from -3 to 3
- down_weight: bfloat16 [5632, 2048], P('tp', 'fs'), may hold values from -0.109375 to 0.109375
Outputs:
- layer_out: bfloat16 [12288, 2048], P('fs', 'tp')
The draws below stay inside these ranges and needn't reach their ends.
All inputs are finite; a program needn't handle non-finite values.
Results may differ from the reference program's by a relative error of at most 0.02.
Values may be sent and summed in bfloat16 or wider, within the bound.
No kernel may reach another device: no remote copies, remote signals or barrier semaphores. Data moves between devices by JAX's collectives and lax.ppermute only.
A program may use at most 128 MiB of HBM per device.

```python
import jax
import jax.numpy as jnp
from jax import lax

D = 2048
HEADS = 8
DK = 256
DV = 512
FF = 5632
KW = 3
BLOCK = 128
SEQ_LEN = 768
TOKENS = 12288
N_TP = 8


def draw_decay_logs(key, part):
    pick_key = jax.random.fold_in(key, 11)
    fast_key = jax.random.fold_in(key, 12)
    slow_key = jax.random.fold_in(key, 13)
    order = jax.random.permutation(pick_key, HEADS)
    quick = order < HEADS // 2
    fast = -1.0 / jax.random.uniform(fast_key, (HEADS,), jnp.float32, 30.0, 100.0)
    slow = -jax.random.uniform(slow_key, (HEADS,), jnp.float32, 0.3, 2.0) / SEQ_LEN
    return jnp.where(quick, fast, slow).astype(jnp.float32)


def strengthened(array, own_key, source, target, blocks, factor):
    def block_of(dim):
        return (jnp.arange(array.shape[dim]) // (array.shape[dim] // blocks)).reshape((-1,) + (1,) * (array.ndim - 1 - dim))

    one_side = jax.random.permutation(own_key, blocks)[block_of(target)]
    far = (block_of(target) + blocks // 2) % blocks
    return jnp.where((block_of(source) == one_side) | (block_of(source) == far), factor * array, array)


def levels(key, shape, split, least, high):
    level, own = 1.0, jax.random.fold_in(key, 6)
    for dim, parts in split:
        heights = jnp.exp(jax.random.uniform(jax.random.fold_in(own, dim), (parts,), jnp.float32, least / len(split), high / len(split)))
        level = level * jnp.repeat(heights, shape[dim] // parts).reshape([-1 if axis == dim else 1 for axis in range(len(shape))])
    return level


def scatter_about(rng, shape, scale, most, pieces=(), kind=jnp.bfloat16):
    gain = levels(rng, shape, pieces, -0.22, 0.18) if pieces else 1.0
    values = jax.random.normal(rng, shape, jnp.float32) * scale * gain
    return jnp.minimum(jnp.maximum(values, -most), most).astype(kind)


def noise_with(own_key, dims, scale, limit, split, heavy, kind=jnp.bfloat16):
    drawn = scale * jax.random.normal(own_key, dims, jnp.float32)
    if split:
        drawn = drawn * levels(own_key, dims, split, -0.22, 0.18)
    return jnp.clip(strengthened(drawn, jax.random.fold_in(own_key, 3), *heavy), -limit, limit).astype(kind)


def setup_inputs(seed: int = 0) -> dict:
    keys = jax.random.split(jax.random.key(seed), 14)
    seq_rows = scatter_about(keys[0], (TOKENS, D), 1.0, 6.0, ((0, 16), (1, 8)))
    mixer_gain = jnp.clip(1.0 + 0.18 * jax.random.normal(keys[1], (D,), jnp.float32), 0.099609375, 1.8984375).astype(jnp.bfloat16)
    query_weight = scatter_about(keys[2], (D, HEADS * DK), D ** -0.5, 0.125, ((0, 16), (1, 8)))
    key_weight = scatter_about(keys[3], (D, HEADS * DK), D ** -0.5, 0.125, ((0, 16), (1, 8)))
    value_weight = scatter_about(keys[4], (D, HEADS * DV), D ** -0.5, 0.125, ((0, 16), (1, 8)))
    decay_logs = draw_decay_logs(jax.random.fold_in(keys[13], 71), 0)
    mixer_out_weight = noise_with(keys[6], (HEADS * DV, D), (HEADS * DV) ** -0.5, 0.125, ((0, 8), (1, 16)), (0, 1, 16, 2.0))
    channel_gain = jnp.clip(1.0 + 0.18 * jax.random.normal(keys[7], (D,), jnp.float32), 0.099609375, 1.8984375).astype(jnp.bfloat16)
    value_up_weight = scatter_about(keys[8], (D, FF), D ** -0.5, 0.125, ((0, 16), (1, 8)))
    gate_up_weight = scatter_about(keys[9], (D, FF), D ** -0.5, 0.125, ((0, 16), (1, 8)))
    conv_taps = scatter_about(keys[10], (KW, FF), 0.6, 3.0, ((1, 8),))
    conv_bias = scatter_about(keys[11], (FF,), 0.5, 3.0, ((0, 8),))
    down_weight = noise_with(keys[12], (FF, D), FF ** -0.5, 0.109375, ((0, 8), (1, 16)), (0, 1, 16, 2.0))
    return dict(seq_rows=seq_rows, mixer_gain=mixer_gain, query_weight=query_weight, key_weight=key_weight, value_weight=value_weight, decay_logs=decay_logs, mixer_out_weight=mixer_out_weight, channel_gain=channel_gain, value_up_weight=value_up_weight, gate_up_weight=gate_up_weight, conv_taps=conv_taps, conv_bias=conv_bias, down_weight=down_weight)


EPS = 1e-06
ROPE_BASE = 10000.0
HIGH_PRECISION = lax.Precision.HIGHEST

def rotate_heads(tensor, cosine, sine):
    half = tensor.shape[-1] // 2
    first = tensor[..., :half]
    second = tensor[..., half:]
    return jnp.concatenate([first * cosine - second * sine, first * sine + second * cosine], axis=-1)

def retention_blocks(query, key, value, decay_logs):
    length, heads = (query.shape[0], query.shape[1])
    count = length // BLOCK
    offsets = jnp.arange(BLOCK, dtype=jnp.float32)
    spread = offsets[:, None] - offsets[None, :]
    within_block = jnp.where(spread[None] >= 0.0, jnp.exp(decay_logs[:, None, None] * jnp.maximum(spread, 0.0)[None]), 0.0)
    carried = jnp.exp(decay_logs[:, None] * (offsets + 1.0))
    state_decay_factor = jnp.exp(decay_logs[:, None] * (BLOCK - 1.0 - offsets))
    block_decay_factor = jnp.exp(decay_logs * BLOCK)

    def blocks(tensor):
        return tensor.reshape(count, BLOCK, heads, tensor.shape[-1]).transpose(0, 2, 1, 3)

    def advance(recurrent_state, triple):
        query_block, key_block, value_block = triple
        attention_scores = jnp.einsum('ucf,uxf->ucx', query_block, key_block, precision=HIGH_PRECISION) * within_block
        result = jnp.einsum('hnm,hmv->hnv', attention_scores, value_block, precision=HIGH_PRECISION)
        result = result + jnp.einsum('hnd,hdv->hnv', query_block, recurrent_state, precision=HIGH_PRECISION) * carried[:, :, None]
        recurrent_state = block_decay_factor[:, None, None] * recurrent_state + jnp.einsum('ieb,iez->ibz', key_block * state_decay_factor[:, :, None], value_block, precision=HIGH_PRECISION)
        return (recurrent_state, result)
    start = jnp.zeros((heads, query.shape[-1], value.shape[-1]), jnp.float32)
    _, result = lax.scan(advance, start, (blocks(query), blocks(key), blocks(value)))
    return result.transpose(0, 2, 1, 3).reshape(length, heads, value.shape[-1])

def grouped_sum(left, right, groups):
    width = left.shape[1] // groups

    def add_group(index, total):
        begin = (index * width).astype(jnp.int32)
        term = jnp.dot(lax.dynamic_slice_in_dim(left, begin, width, 1), lax.dynamic_slice_in_dim(right, begin, width, 0), preferred_element_type=jnp.float32)
        rounded = lax.optimization_barrier(term.astype(jnp.bfloat16))
        return total + rounded.astype(jnp.float32)
    start = jnp.zeros((left.shape[0], right.shape[1]), jnp.float32)
    return lax.fori_loop(jnp.int32(0), jnp.int32(groups), add_group, start)

def one_sequence(rows, mixer_gain, query_weight, key_weight, value_weight, decay_logs, mixer_out_weight, channel_gain, value_up_weight, gate_up_weight, conv_taps, conv_bias, down_weight):
    length = rows.shape[0]
    rows_f = rows.astype(jnp.float32)
    scale_one = lax.rsqrt(lax.optimization_barrier(jnp.mean(rows_f * rows_f, axis=-1, keepdims=True)) + EPS)
    scaled_one = (rows_f * mixer_gain.astype(jnp.float32)).astype(jnp.bfloat16)
    query = (jnp.dot(scaled_one, query_weight, preferred_element_type=jnp.float32) * scale_one).astype(jnp.bfloat16)
    key = (jnp.dot(scaled_one, key_weight, preferred_element_type=jnp.float32) * scale_one).astype(jnp.bfloat16)
    value = (jnp.dot(scaled_one, value_weight, preferred_element_type=jnp.float32) * scale_one).astype(jnp.bfloat16)
    half = DK // 2
    freqs = jnp.power(ROPE_BASE, -jnp.arange(half, dtype=jnp.float32) * 2.0 / DK)
    angles = jnp.arange(length, dtype=jnp.float32)[:, None] * freqs[None, :]
    cosine = jnp.cos(angles)[:, None, :]
    sine = jnp.sin(angles)[:, None, :]
    turned_q = rotate_heads(query.astype(jnp.float32).reshape(length, HEADS, DK), cosine, sine)
    turned_k = rotate_heads(key.astype(jnp.float32).reshape(length, HEADS, DK), cosine, sine) * DK ** (-0.5)
    ret = retention_blocks(turned_q, turned_k, value.astype(jnp.float32).reshape(length, HEADS, DV), decay_logs)
    centred = ret - lax.optimization_barrier(jnp.mean(ret, axis=-1, keepdims=True))
    normed = (centred * lax.rsqrt(lax.optimization_barrier(jnp.mean(centred * centred, axis=-1, keepdims=True)) + EPS)).reshape(length, HEADS * DV).astype(jnp.bfloat16)
    mixed = grouped_sum(normed, mixer_out_weight, N_TP)
    middle = (rows_f + mixed).astype(jnp.bfloat16)
    middle_f = middle.astype(jnp.float32)
    scale_two = lax.rsqrt(lax.optimization_barrier(jnp.mean(middle_f * middle_f, axis=-1, keepdims=True)) + EPS)
    scaled_two = (middle_f * channel_gain.astype(jnp.float32)).astype(jnp.bfloat16)
    up_val = (jnp.dot(scaled_two, value_up_weight, preferred_element_type=jnp.float32) * scale_two).astype(jnp.bfloat16)
    up_gate = (jnp.dot(scaled_two, gate_up_weight, preferred_element_type=jnp.float32) * scale_two).astype(jnp.bfloat16)
    padded = jnp.concatenate([jnp.zeros((KW - 1, FF), jnp.float32), up_gate.astype(jnp.float32)], axis=0)
    conv = jnp.zeros((length, FF), jnp.float32) + conv_bias.astype(jnp.float32)[None, :]
    for tap in range(KW):
        conv = conv + conv_taps[tap].astype(jnp.float32)[None, :] * padded[tap:tap + length]
    hidden = (jax.nn.silu(conv) * up_val.astype(jnp.float32)).astype(jnp.bfloat16)
    channel = grouped_sum(hidden, down_weight, N_TP)
    return (middle_f + channel).astype(jnp.bfloat16)

def reference(seq_rows, mixer_gain, query_weight, key_weight, value_weight, decay_logs, mixer_out_weight, channel_gain, value_up_weight, gate_up_weight, conv_taps, conv_bias, down_weight):
    sequences = seq_rows.reshape(TOKENS // SEQ_LEN, SEQ_LEN, D)

    def run(rows):
        return one_sequence(rows, mixer_gain, query_weight, key_weight, value_weight, decay_logs, mixer_out_weight, channel_gain, value_up_weight, gate_up_weight, conv_taps, conv_bias, down_weight)
    return lax.map(run, sequences).reshape(TOKENS, D)
```

```python
import numpy as np
import jax
import jax.numpy as jnp
from jax import lax
from jax.experimental import pallas as pl
from jax.experimental.pallas import tpu as pltpu
from jax.sharding import Mesh
from jax.sharding import PartitionSpec as P

DK = 256
DV = 512
KW = 3
D = 2048
SEQ = 768
FH = 704
ROWS = 256
STEPS = SEQ // ROWS
TP = ("y", "c")
FS = ("z", "x")
EPS = 1e-06
ROPE_BASE = 10000.0
OFF = (0, 1, 3, 2)
F32 = jnp.float32
BF16 = jnp.bfloat16
ANY = pl.BlockSpec(memory_space=pl.ANY)


def fetch(a, axis, offset):
    n = lax.axis_size(axis)
    return lax.ppermute(a, axis, [(i, (i - offset) % n) for i in range(n)])


def sds(shape, dtype):
    return jax.ShapeDtypeStruct(shape, dtype)


def cost(flops, nbytes):
    return pl.CostEstimate(flops=flops, bytes_accessed=nbytes, transcendentals=0)


def pack_rows(x, gains, wq, wk):
    def body(x_ref, g_ref, wq_ref, wk_ref, xg_ref, wqk_ref, pad, sems):
        copies = [
            pltpu.make_async_copy(x_ref, xg_ref.at[pl.ds(0, SEQ)], sems.at[0]),
            pltpu.make_async_copy(wq_ref, wqk_ref.at[:, pl.ds(0, DK)], sems.at[1]),
            pltpu.make_async_copy(wk_ref, wqk_ref.at[:, pl.ds(DK, DK)], sems.at[2]),
        ]
        for c in copies:
            c.start()
        g = g_ref[...].astype(F32)
        row = lax.broadcasted_iota(jnp.int32, (16, 256), 0)
        pad[...] = jnp.where(row == 0, g[0:1], g[1:2]).astype(BF16)
        last = pltpu.make_async_copy(pad, xg_ref.at[pl.ds(SEQ, 16)], sems.at[3])
        last.start()
        for c in copies:
            c.wait()
        last.wait()

    return pl.pallas_call(
        body,
        in_specs=[ANY, pl.BlockSpec(memory_space=pltpu.VMEM), ANY, ANY],
        out_specs=[ANY, ANY],
        out_shape=[sds((SEQ + 16, 256), BF16), sds((128, 2 * DK), BF16)],
        scratch_shapes=[pltpu.VMEM((16, 256), BF16), pltpu.SemaphoreType.DMA((4,))],
        name="pack_rows",
    )(x, gains, wq, wk)


def stack4(parts):
    shape = parts[0].shape

    def body(a, b, c, d, out, sems):
        copies = [pltpu.make_async_copy(r, out.at[k], sems.at[k]) for k, r in enumerate((a, b, c, d))]
        for c in copies:
            c.start()
        for c in copies:
            c.wait()

    return pl.pallas_call(
        body,
        in_specs=[ANY] * 4,
        out_specs=ANY,
        out_shape=sds((4, *shape), BF16),
        scratch_shapes=[pltpu.SemaphoreType.DMA((4,))],
        name="stack4",
    )(*parts)


def gathered(shard, first, second):
    near = stack4([shard] + [fetch(shard, first, o) for o in OFF[1:]])
    return [near] + [fetch(near, second, o) for o in OFF[1:]]


def relative_place(z, x):
    fs = z * 4 + x
    owner = fs // 2
    turn = (owner // 2 - lax.axis_index("y") + 4) % 4
    other = jnp.where(owner % 2 == lax.axis_index("c"), 0, 4)
    return pl.multiple_of((other + turn) * 256 + (fs % 2) * 128, 128)


def shard_copies(parts, first, place, sems, base):
    me_z, me_x = lax.axis_index("z"), lax.axis_index("x")
    copies = []
    for far, ref in enumerate(parts):
        for near in range(4):
            if first == "x":
                z, x = (me_z + OFF[far]) % 4, (me_x + OFF[near]) % 4
            else:
                z, x = (me_z + OFF[near]) % 4, (me_x + OFF[far]) % 4
            copies.append(
                pltpu.make_async_copy(
                    ref.at[near], place(relative_place(z, x)), sems.at[base + far * 4 + near]
                )
            )
    return copies


def normalise(blocks, gain_blocks, which):
    def body(*refs):
        xs, gs, (out, factor) = refs[:8], refs[8:16], refs[16:]
        total = jnp.zeros((ROWS, 128), F32)
        for b in range(8):
            x = xs[b][...].astype(F32)
            sq = x * x
            total = total + sq[:, :128] + sq[:, 128:]
            gain = gs[b][...].astype(F32)[which : which + 1]
            out[:, b * 256 : (b + 1) * 256] = (x * gain).astype(BF16)
        mean = jnp.sum(total, axis=-1, keepdims=True) * (1.0 / D)
        factor[...] = jnp.broadcast_to(lax.rsqrt(mean + EPS), (ROWS, 128))

    return pl.pallas_call(
        body,
        grid=(STEPS,),
        in_specs=[pl.BlockSpec((ROWS, 256), lambda i: (i, 0))] * 8
        + [pl.BlockSpec((16, 256), lambda i: (SEQ // 16, 0))] * 8,
        out_specs=[
            pl.BlockSpec((ROWS, D), lambda i: (i, 0)),
            pl.BlockSpec((ROWS, 128), lambda i: (i, 0)),
        ],
        out_shape=[sds((SEQ, D), BF16), sds((SEQ, 128), F32)],
        name="normalise",
    )(*blocks, *gain_blocks)


def retention(scaled, factor, cosine, sine, decay, qk_parts, v_parts):
    def body(decay_ref, x_ref, f_ref, cos_ref, sin_ref, *rest):
        qk_refs, v_refs = rest[:4], rest[4:8]
        out_ref, wqk, wv, keys, values, sems = rest[8:]
        step = pl.program_id(0)

        @pl.when(step == 0)
        def _():
            copies = shard_copies(
                qk_refs, "x", lambda p: wqk.at[pl.ds(p, 128)], sems, 0
            ) + shard_copies(v_refs, "z", lambda p: wv.at[pl.ds(p, 128)], sems, 16)
            for c in copies:
                c.start()
            for c in copies:
                c.wait()

        x = x_ref[...]
        f = f_ref[...]
        qk = jnp.dot(x, wqk[...], preferred_element_type=F32)
        v = jnp.dot(x, wv[...], preferred_element_type=F32)
        cos, sin = cos_ref[...], sin_ref[...]

        def turned(m):
            a = (m[:, :128] * f).astype(BF16).astype(F32)
            b = (m[:, 128:] * f).astype(BF16).astype(F32)
            return jnp.concatenate([a * cos - b * sin, a * sin + b * cos], axis=1)

        q = turned(qk[:, :DK]).astype(BF16)
        k = (turned(qk[:, DK:]) * DK**-0.5).astype(BF16)
        v = (v * f[:, :1]).astype(BF16)
        log_g = decay_ref[0]

        for s in range(STEPS):

            @pl.when(step == s)
            def _():
                width = (s + 1) * ROWS
                keys[s * ROWS : width] = k
                values[s * ROWS : width] = v
                scores = lax.dot_general(
                    q, keys[:width], (((1,), (1,)), ((), ())), preferred_element_type=F32
                )
                apart = (
                    lax.broadcasted_iota(jnp.int32, (ROWS, width), 0)
                    + s * ROWS
                    - lax.broadcasted_iota(jnp.int32, (ROWS, width), 1)
                )
                decayed = jnp.exp(log_g * jnp.maximum(apart, 0).astype(F32))
                scores = jnp.where(apart >= 0, scores * decayed, 0.0).astype(BF16)
                ret = jnp.dot(scores, values[:width], preferred_element_type=F32)
                centred = ret - jnp.mean(ret, axis=-1, keepdims=True)
                spread = jnp.mean(centred * centred, axis=-1, keepdims=True)
                out_ref[...] = (centred * lax.rsqrt(spread + EPS)).astype(BF16)

    return pl.pallas_call(
        body,
        grid=(STEPS,),
        in_specs=[
            pl.BlockSpec(memory_space=pltpu.SMEM),
            pl.BlockSpec((ROWS, D), lambda i: (i, 0)),
            pl.BlockSpec((ROWS, 128), lambda i: (i, 0)),
            pl.BlockSpec((ROWS, 128), lambda i: (i, 0)),
            pl.BlockSpec((ROWS, 128), lambda i: (i, 0)),
        ]
        + [ANY] * 8,
        out_specs=pl.BlockSpec((ROWS, DV), lambda i: (i, 0)),
        out_shape=sds((SEQ, DV), BF16),
        scratch_shapes=[
            pltpu.VMEM((D, 2 * DK), BF16),
            pltpu.VMEM((D, DV), BF16),
            pltpu.VMEM((SEQ, DK), BF16),
            pltpu.VMEM((SEQ, DV), BF16),
            pltpu.SemaphoreType.DMA((32,)),
        ],
        cost_estimate=cost(4_000_000_000, 8_000_000),
        compiler_params=pltpu.CompilerParams(vmem_limit_bytes=40 * 2**20),
        name="retention",
    )(decay, scaled, factor, cosine, sine, *qk_parts, *v_parts)


def project(left, parts, first):
    inner = left.shape[1]

    def body(l_ref, *rest):
        refs, (keep, give, w, sems) = rest[:4], rest[4:]

        @pl.when(pl.program_id(0) == 0)
        def _():
            copies = shard_copies(refs, first, lambda p: w.at[:, pl.ds(p, 128)], sems, 0)
            for c in copies:
                c.start()
            for c in copies:
                c.wait()

        left_rows = l_ref[...]
        for b in range(8):
            block = jnp.dot(
                left_rows, w[:, b * 256 : (b + 1) * 256], preferred_element_type=F32
            ).astype(BF16)
            if b < 4:
                keep[b] = block
            else:
                give[b - 4] = block

    spec = pl.BlockSpec((4, ROWS, 256), lambda i: (0, i, 0))
    return pl.pallas_call(
        body,
        grid=(STEPS,),
        in_specs=[pl.BlockSpec((ROWS, inner), lambda i: (i, 0))] + [ANY] * 4,
        out_specs=[spec, spec],
        out_shape=[sds((4, SEQ, 256), BF16)] * 2,
        scratch_shapes=[pltpu.VMEM((inner, D), BF16), pltpu.SemaphoreType.DMA((16,))],
        cost_estimate=cost(2 * SEQ * inner * D, 6_000_000),
        name="project",
    )(left, *parts)


def pair_sum(keep, got):
    def body(k, g, *outs):
        for j in range(3):
            outs[j][...] = (k[j + 1].astype(F32) + g[j + 1].astype(F32)).astype(BF16)

    spec = pl.BlockSpec((4, ROWS, 256), lambda i: (0, i, 0))
    return pl.pallas_call(
        body,
        grid=(STEPS,),
        in_specs=[spec, spec],
        out_specs=[pl.BlockSpec((ROWS, 256), lambda i: (i, 0))] * 3,
        out_shape=[sds((SEQ, 256), BF16)] * 3,
        name="pair_sum",
    )(keep, got)


def final_sum(base, keep, got, arrived):
    def body(x, k, g, a, b, c, out):
        total = k[0].astype(F32) + g[0].astype(F32)
        total = total + a[...].astype(F32) + b[...].astype(F32) + c[...].astype(F32)
        out[...] = (x[...].astype(F32) + total).astype(BF16)

    one = pl.BlockSpec((1, ROWS, 256), lambda i: (0, i, 0))
    row = pl.BlockSpec((ROWS, 256), lambda i: (i, 0))
    return pl.pallas_call(
        body,
        grid=(STEPS,),
        in_specs=[row, one, one, row, row, row],
        out_specs=row,
        out_shape=sds((SEQ, 256), BF16),
        name="final_sum",
    )(base, keep, got, *arrived)


def mixer_hidden(scaled, factor, taps, bias, val_parts, gate_parts):
    def body(x_ref, f_ref, t_ref, b_ref, *rest):
        val_refs, gate_refs = rest[:4], rest[4:8]
        out_ref, wval, wgate, held, sems = rest[8:]
        step = pl.program_id(0)

        @pl.when(step == 0)
        def _():
            copies = shard_copies(
                gate_refs, "z", lambda p: wgate.at[pl.ds(p, 128)], sems, 16
            ) + shard_copies(val_refs, "x", lambda p: wval.at[pl.ds(p, 128)], sems, 0)
            for c in copies:
                c.start()
            held[0:8] = jnp.zeros((8, FH), F32)
            for c in copies:
                c.wait()

        x = x_ref[...]
        f = f_ref[:, :1]
        gate = (jnp.dot(x, wgate[...], preferred_element_type=F32) * f).astype(BF16).astype(F32)
        held[8 : 8 + ROWS] = gate
        taps = t_ref[...].astype(F32)
        conv = b_ref[...].astype(F32) + taps[2:3] * gate
        conv = conv + taps[1:2] * held[7 : 7 + ROWS]
        conv = conv + taps[0:1] * held[6 : 6 + ROWS]
        held[0:8] = held[ROWS : ROWS + 8]
        val = (jnp.dot(x, wval[...], preferred_element_type=F32) * f).astype(BF16).astype(F32)
        out_ref[...] = (conv / (1.0 + jnp.exp(-conv)) * val).astype(BF16)

    return pl.pallas_call(
        body,
        grid=(STEPS,),
        in_specs=[
            pl.BlockSpec((ROWS, D), lambda i: (i, 0)),
            pl.BlockSpec((ROWS, 128), lambda i: (i, 0)),
            pl.BlockSpec((KW, FH), lambda i: (0, 0)),
            pl.BlockSpec((1, FH), lambda i: (0, 0)),
        ]
        + [ANY] * 8,
        out_specs=pl.BlockSpec((ROWS, FH), lambda i: (i, 0)),
        out_shape=sds((SEQ, FH), BF16),
        scratch_shapes=[
            pltpu.VMEM((D, FH), BF16),
            pltpu.VMEM((D, FH), BF16),
            pltpu.VMEM((ROWS + 8, FH), F32),
            pltpu.SemaphoreType.DMA((32,)),
        ],
        cost_estimate=cost(4_500_000_000, 9_000_000),
        compiler_params=pltpu.CompilerParams(vmem_limit_bytes=40 * 2**20),
        name="mixer_hidden",
    )(scaled, factor, taps, bias, *val_parts, *gate_parts)


def all_features(block):
    same = [block] + [fetch(block, "y", j) for j in (1, 2, 3)]
    return same + [fetch(b, "c", 1) for b in same]


def to_owners(base, keep, give):
    got = fetch(give, "c", 1)
    sums = pair_sum(keep, got)
    arrived = [fetch(s, "y", -(j + 1)) for j, s in enumerate(sums)]
    return final_sum(base, keep, got, arrived)


def rotation_tables():
    freqs = ROPE_BASE ** (-np.arange(DK // 2, dtype=np.float64) * 2.0 / DK)
    angles = np.arange(SEQ, dtype=np.float64)[:, None] * freqs[None, :]
    return np.cos(angles).astype(np.float32), np.sin(angles).astype(np.float32)


def on_device(
    seq_rows,
    mixer_gain,
    query_weight,
    key_weight,
    value_weight,
    decay_logs,
    mixer_out_weight,
    channel_gain,
    value_up_weight,
    gate_up_weight,
    conv_taps,
    conv_bias,
    down_weight,
):
    rows_gain, wqk = pack_rows(
        seq_rows, jnp.stack([mixer_gain, channel_gain]), query_weight, key_weight
    )
    blocks = all_features(rows_gain)
    qk_parts = gathered(wqk, "x", "z")
    v_parts = gathered(value_weight, "z", "x")
    out_parts = gathered(mixer_out_weight, "x", "z")
    val_parts = gathered(value_up_weight, "x", "z")
    gate_parts = gathered(gate_up_weight, "z", "x")
    down_parts = gathered(down_weight, "z", "x")

    cosine, sine = rotation_tables()
    scaled, factor = normalise(blocks, blocks, 0)
    normed = retention(
        scaled, factor, jnp.asarray(cosine), jnp.asarray(sine), decay_logs, qk_parts, v_parts
    )
    middle = to_owners(seq_rows, *project(normed, out_parts, "x"))

    scaled, factor = normalise(all_features(middle), blocks, 1)
    hidden = mixer_hidden(
        scaled, factor, conv_taps, conv_bias.reshape(1, FH), val_parts, gate_parts
    )
    return to_owners(middle, *project(hidden, down_parts, "z"))


def solution(mesh):
    torus = Mesh(mesh.devices.reshape(4, 4, 4, 2), ("z", "x", "y", "c"))
    return jax.shard_map(
        on_device,
        mesh=torus,
        in_specs=(
            P(FS, TP),
            P(TP),
            P(FS, TP),
            P(FS, TP),
            P(FS, TP),
            P(TP),
            P(TP, FS),
            P(TP),
            P(FS, TP),
            P(FS, TP),
            P(None, TP),
            P(TP),
            P(TP, FS),
        ),
        out_specs=P(FS, TP),
        check_vma=False,
    )
```

```python
import numpy as np
import jax
import jax.numpy as jnp
from jax import lax
from jax.experimental import pallas as pl
from jax.experimental.pallas import tpu as pltpu
from jax.sharding import Mesh
from jax.sharding import PartitionSpec as P

DK = 256
DV = 512
KW = 3
D = 2048
SEQ = 768
FH = 704
ROWS = 256
STEPS = SEQ // ROWS
TP = ("y", "c")
FS = ("z", "x")
EPS = 1e-06
ROPE_BASE = 10000.0
OFF = (0, 1, 3, 2)
F32 = jnp.float32
BF16 = jnp.bfloat16
ANY = pl.BlockSpec(memory_space=pl.ANY)


def fetch(a, axis, offset):
    n = lax.axis_size(axis)
    return lax.ppermute(a, axis, [(i, (i - offset) % n) for i in range(n)])


def sds(shape, dtype):
    return jax.ShapeDtypeStruct(shape, dtype)


def cost(flops, nbytes):
    return pl.CostEstimate(flops=flops, bytes_accessed=nbytes, transcendentals=0)


def vmem_call(body, name, out_shape, *operands, mib=8, scratch=()):
    whole = pl.BlockSpec(memory_space=pltpu.VMEM)
    return pl.pallas_call(
        body,
        in_specs=[whole] * len(operands),
        out_specs=jax.tree.map(lambda _: whole, out_shape),
        out_shape=out_shape,
        scratch_shapes=scratch,
        compiler_params=pltpu.CompilerParams(vmem_limit_bytes=mib * 2**20),
        name=name,
    )(*operands)


def pack_first(x, gains, wq, wk, wv, wo):
    def body(x_ref, g_ref, q_ref, k_ref, v_ref, o_ref, xg, left, right):
        xg[0:SEQ] = x_ref[...]
        g = g_ref[...].astype(F32)
        row = lax.broadcasted_iota(jnp.int32, (16, 256), 0)
        xg[SEQ : SEQ + 16] = jnp.where(row == 0, g[0:1], g[1:2]).astype(BF16)
        left[:, 0:DK] = q_ref[...]
        left[:, DK : 2 * DK] = k_ref[...]
        right[:, 0:DV] = v_ref[...]
        for h in range(2):
            left[:, DV + h * 128 : DV + h * 128 + 128] = o_ref[h * 128 : h * 128 + 128]
            right[:, DV + h * 128 : DV + h * 128 + 128] = o_ref[256 + h * 128 : 384 + h * 128]

    shapes = (sds((SEQ + 16, 256), BF16), sds((128, 768), BF16), sds((128, 768), BF16))
    return vmem_call(body, "pack_first", shapes, x, gains, wq, wk, wv, wo)


def pack_second(val, gate, down):
    def body(v_ref, g_ref, d_ref, left, right):
        left[0:FH] = v_ref[...]
        left[FH : FH + FH // 2] = g_ref[0 : FH // 2]
        right[0 : FH // 2] = g_ref[FH // 2 : FH]
        right[FH // 2 :] = d_ref[...]

    half = sds((FH + FH // 2, 128), BF16)
    return vmem_call(body, "pack_second", (half, half), val, gate, down)


def stack4(parts):
    def body(a, b, c, d, out):
        for k, r in enumerate((a, b, c, d)):
            out[k] = r[...]

    return vmem_call(body, "stack4", sds((4, *parts[0].shape), BF16), *parts)


def near_gather(shard, axis):
    return stack4([shard] + [fetch(shard, axis, o) for o in OFF[1:]])


def far_gather(near, axis):
    return [near] + [fetch(near, axis, o) for o in OFF[1:]]


def relative_place(z, x):
    fs = z * 4 + x
    owner = fs // 2
    turn = (owner // 2 - lax.axis_index("y") + 4) % 4
    other = jnp.where(owner % 2 == lax.axis_index("c"), 0, 4)
    return pl.multiple_of((other + turn) * 256 + (fs % 2) * 128, 128)


def placed(parts, first):
    me_z, me_x = lax.axis_index("z"), lax.axis_index("x")
    for far, ref in enumerate(parts):
        for near in range(4):
            if first == "x":
                z, x = (me_z + OFF[far]) % 4, (me_x + OFF[near]) % 4
            else:
                z, x = (me_z + OFF[near]) % 4, (me_x + OFF[far]) % 4
            yield ref.at[near], relative_place(z, x)


def send(src, dst, sem):
    pltpu.make_async_copy(src, dst, sem).start()


def wait_all(ref, sem):
    pltpu.make_async_copy(ref, ref, sem).wait()


def scale_rows(xs, gains, which, out):
    total = jnp.zeros((ROWS, 128), F32)
    for b in range(8):
        x = xs[b][...].astype(F32)
        sq = x * x
        total = total + sq[:, :128] + sq[:, 128:]
        gain = gains[b][...].astype(F32)[which : which + 1]
        out[:, b * 256 : (b + 1) * 256] = (x * gain).astype(BF16)
    mean = jnp.sum(total, axis=-1, keepdims=True) * (1.0 / D)
    return lax.rsqrt(mean + EPS)


BLOCKS8 = [pl.BlockSpec((ROWS, 256), lambda i: (i, 0))] * 8
GAINS8 = [pl.BlockSpec((16, 256), lambda i: (SEQ // 16, 0))] * 8
OWNERS = pl.BlockSpec((4, ROWS, 256), lambda i: (0, i, 0))


def normalise(blocks):
    def body(*refs):
        xs, gs, (out, factor) = refs[:8], refs[8:16], refs[16:]
        factor[...] = jnp.broadcast_to(scale_rows(xs, gs, 0, out), (ROWS, 128))

    return pl.pallas_call(
        body,
        grid=(STEPS,),
        in_specs=BLOCKS8 + GAINS8,
        out_specs=[
            pl.BlockSpec((ROWS, D), lambda i: (i, 0)),
            pl.BlockSpec((ROWS, 128), lambda i: (i, 0)),
        ],
        out_shape=[sds((SEQ, D), BF16), sds((SEQ, 128), F32)],
        cost_estimate=cost(500_000_000, 6_000_000),
        compiler_params=pltpu.CompilerParams(vmem_limit_bytes=10 * 2**20),
        name="normalise",
    )(*blocks, *blocks)


def to_blocks(left_rows, w, keep, give):
    for b in range(8):
        block = jnp.dot(
            left_rows, w[:, b * 256 : (b + 1) * 256], preferred_element_type=F32
        ).astype(BF16)
        if b < 4:
            keep[b] = block
        else:
            give[b - 4] = block


def retention(scaled, factor, cosine, sine, decay, left_parts, right_parts):
    def body(decay_ref, x_ref, f_ref, cos_ref, sin_ref, *rest):
        lefts, rights = rest[:4], rest[4:8]
        keep, give, wqk, wv, wo, keys, values, sems = rest[8:]
        step = pl.program_id(0)

        @pl.when(step == 0)
        def _():
            pieces = [(0, p, at) for p, at in placed(lefts, "x")]
            pieces += [(1, p, at) for p, at in placed(rights, "z")]
            for side, piece, at in pieces:
                send(piece.at[:, 0:DV], (wv if side else wqk).at[pl.ds(at, 128)], sems.at[side])
            for side, piece, at in pieces:
                for h in range(2):
                    send(
                        piece.at[:, DV + h * 128 : DV + h * 128 + 128],
                        wo.at[side * 256 + h * 128 : side * 256 + h * 128 + 128, pl.ds(at, 128)],
                        sems.at[2],
                    )
            wait_all(wqk, sems.at[0])
            wait_all(wv, sems.at[1])

        x = x_ref[...]
        f = f_ref[...]
        qk = jnp.dot(x, wqk[...], preferred_element_type=F32)
        v = jnp.dot(x, wv[...], preferred_element_type=F32)
        cos, sin = cos_ref[...], sin_ref[...]

        def turned(m):
            a = (m[:, :128] * f).astype(BF16).astype(F32)
            b = (m[:, 128:] * f).astype(BF16).astype(F32)
            return jnp.concatenate([a * cos - b * sin, a * sin + b * cos], axis=1)

        q = turned(qk[:, :DK]).astype(BF16)
        k = (turned(qk[:, DK:]) * DK**-0.5).astype(BF16)
        v = (v * f[:, :1]).astype(BF16)
        log_g = decay_ref[0]

        @pl.when(step == 0)
        def _():
            wait_all(wo, sems.at[2])

        for s in range(STEPS):

            @pl.when(step == s)
            def _():
                width = (s + 1) * ROWS
                keys[s * ROWS : width] = k
                values[s * ROWS : width] = v
                scores = lax.dot_general(
                    q, keys[:width], (((1,), (1,)), ((), ())), preferred_element_type=F32
                )
                apart = (
                    lax.broadcasted_iota(jnp.int32, (ROWS, width), 0)
                    + s * ROWS
                    - lax.broadcasted_iota(jnp.int32, (ROWS, width), 1)
                )
                decayed = jnp.exp(log_g * jnp.maximum(apart, 0).astype(F32))
                scores = jnp.where(apart >= 0, scores * decayed, 0.0).astype(BF16)
                ret = jnp.dot(scores, values[:width], preferred_element_type=F32)
                centred = ret - jnp.mean(ret, axis=-1, keepdims=True)
                spread = jnp.mean(centred * centred, axis=-1, keepdims=True)
                normed = (centred * lax.rsqrt(spread + EPS)).astype(BF16)
                to_blocks(normed, wo, keep, give)

    return pl.pallas_call(
        body,
        grid=(STEPS,),
        in_specs=[
            pl.BlockSpec(memory_space=pltpu.SMEM),
            pl.BlockSpec((ROWS, D), lambda i: (i, 0)),
            pl.BlockSpec((ROWS, 128), lambda i: (i, 0)),
            pl.BlockSpec((ROWS, 128), lambda i: (i, 0)),
            pl.BlockSpec((ROWS, 128), lambda i: (i, 0)),
        ]
        + [ANY] * 8,
        out_specs=[OWNERS, OWNERS],
        out_shape=[sds((4, SEQ, 256), BF16)] * 2,
        scratch_shapes=[
            pltpu.VMEM((D, 2 * DK), BF16),
            pltpu.VMEM((D, DV), BF16),
            pltpu.VMEM((DV, D), BF16),
            pltpu.VMEM((SEQ, DK), BF16),
            pltpu.VMEM((SEQ, DV), BF16),
            pltpu.SemaphoreType.DMA((3,)),
        ],
        cost_estimate=cost(6_000_000_000, 10_000_000),
        compiler_params=pltpu.CompilerParams(vmem_limit_bytes=24 * 2**20),
        name="retention",
    )(decay, scaled, factor, cosine, sine, *left_parts, *right_parts)


def channel_mixer(blocks, gain_blocks, taps, bias, left_parts, right_parts):
    edge = FH + FH // 2

    def body(*refs):
        xs, gs, (t_ref, b_ref) = refs[:8], refs[8:16], refs[16:18]
        lefts, rights = refs[18:22], refs[22:26]
        keep, give, scaled, wup, wdown, held, sems = refs[26:]
        step = pl.program_id(0)

        @pl.when(step == 0)
        def _():
            later = []
            for piece, at in placed(lefts, "x"):
                send(piece, wup.at[0:edge, pl.ds(at, 128)], sems.at[0])
            for piece, at in placed(rights, "z"):
                send(piece.at[0 : FH // 2], wup.at[edge:, pl.ds(at, 128)], sems.at[1])
                later.append((piece, at))
            for piece, at in later:
                send(piece.at[FH // 2 :], wdown.at[:, pl.ds(at, 128)], sems.at[2])
            held[0:8] = jnp.zeros((8, FH), F32)

        f = scale_rows(xs, gs, 1, scaled)

        @pl.when(step == 0)
        def _():
            wait_all(wup.at[0:edge], sems.at[0])
            wait_all(wup.at[edge:], sems.at[1])

        x = scaled[...]

        def up(rows):
            m = lax.dot_general(x, rows, (((1,), (1,)), ((), ())), preferred_element_type=F32)
            return (m * f).astype(BF16).astype(F32)

        gate = up(wup[FH:])
        held[8 : 8 + ROWS] = gate
        taps = t_ref[...].astype(F32)
        conv = b_ref[...].astype(F32) + taps[2:3] * gate
        conv = conv + taps[1:2] * held[7 : 7 + ROWS]
        conv = conv + taps[0:1] * held[6 : 6 + ROWS]
        held[0:8] = held[ROWS : ROWS + 8]
        val = up(wup[0:FH])
        hidden = (conv / (1.0 + jnp.exp(-conv)) * val).astype(BF16)

        @pl.when(step == 0)
        def _():
            wait_all(wdown, sems.at[2])

        to_blocks(hidden, wdown, keep, give)

    return pl.pallas_call(
        body,
        grid=(STEPS,),
        in_specs=BLOCKS8
        + GAINS8
        + [
            pl.BlockSpec((KW, FH), lambda i: (0, 0)),
            pl.BlockSpec((1, FH), lambda i: (0, 0)),
        ]
        + [ANY] * 8,
        out_specs=[OWNERS, OWNERS],
        out_shape=[sds((4, SEQ, 256), BF16)] * 2,
        scratch_shapes=[
            pltpu.VMEM((ROWS, D), BF16),
            pltpu.VMEM((2 * FH, D), BF16),
            pltpu.VMEM((FH, D), BF16),
            pltpu.VMEM((ROWS + 8, FH), F32),
            pltpu.SemaphoreType.DMA((3,)),
        ],
        cost_estimate=cost(7_000_000_000, 14_000_000),
        compiler_params=pltpu.CompilerParams(vmem_limit_bytes=26 * 2**20),
        name="channel_mixer",
    )(*blocks, *gain_blocks, taps, bias, *left_parts, *right_parts)


def pair_sum(keep, got):
    def body(k, g, *outs):
        for j in range(3):
            outs[j][...] = (k[j + 1].astype(F32) + g[j + 1].astype(F32)).astype(BF16)

    return pl.pallas_call(
        body,
        grid=(STEPS,),
        in_specs=[OWNERS, OWNERS],
        out_specs=[pl.BlockSpec((ROWS, 256), lambda i: (i, 0))] * 3,
        out_shape=[sds((SEQ, 256), BF16)] * 3,
        compiler_params=pltpu.CompilerParams(vmem_limit_bytes=6 * 2**20),
        name="pair_sum",
    )(keep, got)


def final_sum(base, keep, got, arrived):
    def body(x, k, g, a, b, c, out):
        total = k[0].astype(F32) + g[0].astype(F32)
        total = total + a[...].astype(F32) + b[...].astype(F32) + c[...].astype(F32)
        out[...] = (x[...].astype(F32) + total).astype(BF16)

    one = pl.BlockSpec((1, ROWS, 256), lambda i: (0, i, 0))
    row = pl.BlockSpec((ROWS, 256), lambda i: (i, 0))
    return pl.pallas_call(
        body,
        grid=(STEPS,),
        in_specs=[row, one, one, row, row, row],
        out_specs=row,
        out_shape=sds((SEQ, 256), BF16),
        compiler_params=pltpu.CompilerParams(vmem_limit_bytes=4 * 2**20),
        name="final_sum",
    )(base, keep, got, *arrived)


def all_features(block):
    same = [block] + [fetch(block, "y", j) for j in (1, 2, 3)]
    return same + [fetch(b, "c", 1) for b in same]


def to_owners(base, keep, give):
    got = fetch(give, "c", 1)
    sums = pair_sum(keep, got)
    arrived = [fetch(s, "y", -(j + 1)) for j, s in enumerate(sums)]
    return final_sum(base, keep, got, arrived)


def rotation_tables():
    freqs = ROPE_BASE ** (-np.arange(DK // 2, dtype=np.float64) * 2.0 / DK)
    angles = np.arange(SEQ, dtype=np.float64)[:, None] * freqs[None, :]
    return np.cos(angles).astype(np.float32), np.sin(angles).astype(np.float32)


def on_device(
    seq_rows,
    mixer_gain,
    query_weight,
    key_weight,
    value_weight,
    decay_logs,
    mixer_out_weight,
    channel_gain,
    value_up_weight,
    gate_up_weight,
    conv_taps,
    conv_bias,
    down_weight,
):
    rows_gain, left_one, right_one = pack_first(
        seq_rows,
        jnp.stack([mixer_gain, channel_gain]),
        query_weight,
        key_weight,
        value_weight,
        mixer_out_weight,
    )
    blocks = all_features(rows_gain)
    left_near = near_gather(left_one, "x")
    right_near = near_gather(right_one, "z")
    left_parts = far_gather(left_near, "z")
    right_parts = far_gather(right_near, "x")

    left_two, right_two = pack_second(
        value_up_weight.swapaxes(0, 1), gate_up_weight.swapaxes(0, 1), down_weight
    )
    up_left = far_gather(near_gather(left_two, "x"), "z")
    up_right = far_gather(near_gather(right_two, "z"), "x")

    cosine, sine = rotation_tables()
    scaled, factor = normalise(blocks)
    keep, give = retention(
        scaled, factor, jnp.asarray(cosine), jnp.asarray(sine), decay_logs, left_parts, right_parts
    )
    middle = to_owners(seq_rows, keep, give)

    keep, give = channel_mixer(
        all_features(middle), blocks, conv_taps, conv_bias.reshape(1, FH), up_left, up_right
    )
    return to_owners(middle, keep, give)


def solution(mesh):
    torus = Mesh(mesh.devices.reshape(4, 4, 4, 2), ("z", "x", "y", "c"))
    return jax.shard_map(
        on_device,
        mesh=torus,
        in_specs=(
            P(FS, TP),
            P(TP),
            P(FS, TP),
            P(FS, TP),
            P(FS, TP),
            P(TP),
            P(TP, FS),
            P(TP),
            P(FS, TP),
            P(FS, TP),
            P(None, TP),
            P(TP),
            P(TP, FS),
        ),
        out_specs=P(FS, TP),
        check_vma=False,
    )
```
